32 devices in a mesh: fs: 8 (over z, y), tp: 4 (over x, core).
Axes of the slice: x: 2, y: 2, z: 4, core: 2. Of those that a mesh axis runs over, the one named last changes fastest.
Arguments:
- tokens: bfloat16 [6144, 2048], P('fs', 'tp'), may hold values from -40 to 40
- gain_one: float32 [2048], P('tp'), may hold values from 0.1 to 1.9
- w_gate: float32 [2048, 3072], P('fs', 'tp'), may hold values from -0.125 to 0.125
- w_up: float32 [2048, 3072], P('fs', 'tp'), may hold values from -0.125 to 0.125
- w_down: float32 [3072, 2048], P('tp', 'fs'), may hold values from -0.109375 to 0.109375
- scale_gate: float32 [3072], P('tp'), may hold values from 0.5 to 2
- scale_up: float32 [3072], P('tp'), may hold values from 0.5 to 2
- scale_down: float32 [2048], P('tp'), may hold values from 0.5 to 2
- gain_mix: float32 [2048], P('tp'), may hold values from 0.1 to 1.9
- w_query: float32 [2048, 2048], P('fs', 'tp'), may hold values from -0.125 to 0.125
- w_key: float32 [2048, 2048], P('fs', 'tp'), may hold values from -0.125 to 0.125
- w_value: float32 [2048, 2048], P('fs', 'tp'), may hold values from -0.125 to 0.125
- w_outgate: float32 [2048, 2048], P('fs', 'tp'), may hold values from -0.125 to 0.125
- scale_query: float32 [2048], P('tp'), may hold values from 0.5 to 2
- scale_key: float32 [2048], P('tp'), may hold values from 0.5 to 2
- scale_value: float32 [2048], P('tp'), may hold values from 0.5 to 2
- scale_outgate: float32 [2048], P('tp'), may hold values from 0.5 to 2
- ret_gain: float32 [2048], P('tp'), may hold values from 0.1 to 1.9
- decay_rate: float32 [8], P('tp'), may hold values from 0 to 2
- w_mix: float32 [2048, 2048], P('tp', 'fs'), may hold values from -0.125 to 0.125
- scale_mix: float32 [2048], P('tp'), may hold values from 0.5 to 2
- gain_two: float32 [2048], P('tp'), may hold values from 0.1 to 1.9
Outputs:
- layer_out: bfloat16 [6144, 2048], P('fs', 'tp')
The draws below stay inside these ranges and needn't reach their ends.
All inputs are finite; a program needn't handle non-finite values.
Results may differ from the reference program's by a relative error of at most 0.022.
Values may be sent and summed in bfloat16 or wider, within the bound.
No kernel may reach another device: no remote copies, remote signals or barrier semaphores. Data moves between devices by JAX's collectives and lax.ppermute only.
A program may use at most 128 MiB of HBM per device.

```python
import math
import jax
import jax.numpy as jnp
from jax import lax

D = 2048
FF = 3072
HEADS = 8
LEN = 256
BLK = 128
RW = 2048
TOKENS = 6144
N_TP = 4


def draw_tokens(key, part):
    base = jax.random.normal(jax.random.fold_in(key, 13), (TOKENS, D), jnp.float32)
    logs = jax.random.uniform(jax.random.fold_in(key, 14), (TOKENS, 8), jnp.float32, -1.2, 1.2)
    factors = jnp.repeat(jnp.exp(logs), D // 8, axis=1)
    return (base * factors).astype(jnp.bfloat16)


def draw_decay_rate(key, part):
    picks = jax.random.randint(jax.random.fold_in(key, 21), (HEADS,), 0, 2)
    quick = jax.random.uniform(jax.random.fold_in(key, 22), (HEADS,), jnp.float32, 4.0 / BLK, 16.0 / BLK)
    slower = jax.random.uniform(jax.random.fold_in(key, 23), (HEADS,), jnp.float32, 0.3 / LEN, 2.3 / LEN)
    return jnp.where(picks == 1, quick, slower)


def steps_of(rng, extent, split, low, high):
    factor_of, own = 1.0, jax.random.fold_in(rng, 6)
    for position, blocks in split:
        heights = jnp.exp(jax.random.uniform(jax.random.fold_in(own, position), (blocks,), jnp.float32, low / len(split), high / len(split)))
        factor_of = factor_of * jnp.repeat(heights, extent[position] // blocks).reshape([-1 if axis == position else 1 for axis in range(len(extent))])
    return factor_of


def centred(rng, dims, deviation, most, split=(), held_as=jnp.bfloat16):
    array = deviation * jax.random.normal(rng, dims, jnp.float32)
    if split:
        array = array * steps_of(rng, dims, split, -0.22, 0.18)
    return jnp.clip(array, -most, most).astype(held_as)


def setup_inputs(seed: int = 0) -> dict:
    seeds = jax.random.split(jax.random.key(seed), 23)
    tokens = draw_tokens(jax.random.fold_in(seeds[22], 71), 0)
    gain_one = jnp.clip(1.0 + 0.18 * jax.random.normal(seeds[1], (D,), jnp.float32), 0.1, 1.9)
    w_gate = centred(seeds[2], (D, FF), D ** -0.5, 0.125, ((0, 8), (1, 4)), jnp.float32)
    w_up = centred(seeds[3], (D, FF), D ** -0.5, 0.125, ((0, 8), (1, 4)), jnp.float32)
    w_down = centred(seeds[4], (FF, D), FF ** -0.5, 0.109375, ((0, 4), (1, 8)), jnp.float32)
    scale_gate = jnp.clip(jnp.exp(math.log(2.0) - 1.3862944 * jax.random.uniform(seeds[5], (FF,), jnp.float32) ** steps_of(seeds[5], (FF,), ((0, 4),), -0.2, 0.2)), 0.5, 2.0)
    scale_up = jnp.clip(jnp.exp(math.log(2.0) - 1.3862944 * jax.random.uniform(seeds[6], (FF,), jnp.float32) ** steps_of(seeds[6], (FF,), ((0, 4),), -0.2, 0.2)), 0.5, 2.0)
    scale_down = jnp.clip(jnp.exp(math.log(2.0) - 1.3862944 * jax.random.uniform(seeds[7], (D,), jnp.float32) ** steps_of(seeds[7], (D,), ((0, 4),), -0.2, 0.2)), 0.5, 2.0)
    gain_mix = jnp.clip(1.0 + 0.18 * jax.random.normal(seeds[8], (D,), jnp.float32), 0.1, 1.9)
    w_query = centred(seeds[9], (D, RW), D ** -0.5, 0.125, ((0, 8), (1, 4)), jnp.float32)
    w_key = centred(seeds[10], (D, RW), D ** -0.5, 0.125, ((0, 8), (1, 4)), jnp.float32)
    w_value = centred(seeds[11], (D, RW), D ** -0.5, 0.125, ((0, 8), (1, 4)), jnp.float32)
    w_outgate = centred(seeds[12], (D, RW), D ** -0.5, 0.125, ((0, 8), (1, 4)), jnp.float32)
    scale_query = jnp.clip(jnp.exp(math.log(2.0) - 1.3862944 * jax.random.uniform(seeds[13], (RW,), jnp.float32) ** steps_of(seeds[13], (RW,), ((0, 4),), -0.2, 0.2)), 0.5, 2.0)
    scale_key = jnp.clip(jnp.exp(math.log(2.0) - 1.3862944 * jax.random.uniform(seeds[14], (RW,), jnp.float32) ** steps_of(seeds[14], (RW,), ((0, 4),), -0.2, 0.2)), 0.5, 2.0)
    scale_value = jnp.clip(jnp.exp(math.log(2.0) - 1.3862944 * jax.random.uniform(seeds[15], (RW,), jnp.float32) ** steps_of(seeds[15], (RW,), ((0, 4),), -0.2, 0.2)), 0.5, 2.0)
    scale_outgate = jnp.clip(jnp.exp(math.log(2.0) - 1.3862944 * jax.random.uniform(seeds[16], (RW,), jnp.float32) ** steps_of(seeds[16], (RW,), ((0, 4),), -0.2, 0.2)), 0.5, 2.0)
    ret_gain = jnp.clip(1.0 + 0.18 * jax.random.normal(seeds[17], (RW,), jnp.float32), 0.1, 1.9)
    decay_rate = draw_decay_rate(jax.random.fold_in(seeds[22], 71), 0)
    w_mix = centred(seeds[19], (RW, D), RW ** -0.5, 0.125, ((0, 4), (1, 8)), jnp.float32)
    scale_mix = jnp.clip(jnp.exp(math.log(2.0) - 1.3862944 * jax.random.uniform(seeds[20], (D,), jnp.float32) ** steps_of(seeds[20], (D,), ((0, 4),), -0.2, 0.2)), 0.5, 2.0)
    gain_two = jnp.clip(1.0 + 0.18 * jax.random.normal(seeds[21], (D,), jnp.float32), 0.1, 1.9)
    return dict(tokens=tokens, gain_one=gain_one, w_gate=w_gate, w_up=w_up, w_down=w_down, scale_gate=scale_gate, scale_up=scale_up, scale_down=scale_down, gain_mix=gain_mix, w_query=w_query, w_key=w_key, w_value=w_value, w_outgate=w_outgate, scale_query=scale_query, scale_key=scale_key, scale_value=scale_value, scale_outgate=scale_outgate, ret_gain=ret_gain, decay_rate=decay_rate, w_mix=w_mix, scale_mix=scale_mix, gain_two=gain_two)


EPS = 1e-06
HEAD_EPS = 0.1

def rms_rows(hidden_in, norm_gain):
    widened = hidden_in.astype(jnp.float32)
    scaled = widened * lax.rsqrt(lax.optimization_barrier(jnp.mean(widened * widened, axis=1, keepdims=True)) + EPS) * norm_gain
    return scaled.astype(jnp.bfloat16)

def project(features, weight, column_scale):
    return jnp.dot(features, weight.astype(jnp.bfloat16), preferred_element_type=jnp.float32) * column_scale

def split_sum(left, weight, parts):
    width = left.shape[1] // parts

    def add_block(index, total):
        start = (index * width).astype(jnp.int32)
        columns = lax.dynamic_slice_in_dim(left, start, width, 1)
        block = lax.dynamic_slice_in_dim(weight, start, width, 0).astype(jnp.bfloat16)
        partial_value = jnp.dot(columns, block, preferred_element_type=jnp.float32).astype(jnp.bfloat16)
        partial_value = lax.optimization_barrier(partial_value)
        return total + partial_value.astype(jnp.float32)
    return lax.fori_loop(0, parts, add_block, jnp.zeros((left.shape[0], weight.shape[1]), jnp.float32))

def feed_forward(features, w_gate, w_up, w_down, scale_gate, scale_up, scale_down):
    gate_pre = project(features, w_gate, scale_gate)
    up_pre = project(features, w_up, scale_up)
    hidden = (jax.nn.silu(gate_pre) * up_pre).astype(jnp.bfloat16)
    return split_sum(hidden, w_down, N_TP) * scale_down

def rotate_pairs(values):
    paired = values.reshape(values.shape[:-1] + (values.shape[-1] // 2, 2))
    return jnp.stack((-paired[..., 1], paired[..., 0]), axis=-1).reshape(values.shape)

def retain(query_rows, key_rows, value_rows, decay_rate, length, block):
    highest = lax.Precision.HIGHEST
    total_rows = query_rows.shape[0]
    heads = decay_rate.shape[0]
    head_size = query_rows.shape[1] // heads
    sequences = total_rows // length
    nblocks = length // block

    def split_heads(values):
        return values.astype(jnp.float32).reshape(sequences, length, heads, head_size)
    freq = 1.0 / 10000.0 ** jnp.linspace(0.0, 1.0, head_size // 2, dtype=jnp.float32)
    freq = jnp.repeat(freq, 2)
    angles = jnp.arange(length, dtype=jnp.float32)[:, None] * freq[None, :]
    sines = jnp.sin(angles)[None, :, None, :]
    cosines = jnp.cos(angles)[None, :, None, :]
    queries = split_heads(query_rows)
    queries = queries * cosines + rotate_pairs(queries) * sines
    keys_all = split_heads(key_rows) * head_size ** (-0.5)
    keys_all = keys_all * cosines + rotate_pairs(keys_all) * sines
    values_all = split_heads(value_rows)
    log_decay = -decay_rate.astype(jnp.float32)
    offsets = jnp.arange(block, dtype=jnp.float32)
    distance = offsets[:, None] - offsets[None, :]
    inside = jnp.where(distance >= 0, jnp.exp(log_decay[:, None, None] * jnp.maximum(distance, 0.0)), 0.0)
    query_decay = jnp.exp(log_decay[None, :] * (offsets[:, None] + 1.0))
    key_decay = jnp.exp(log_decay[None, :] * (block - 1.0 - offsets[:, None]))
    block_decay = jnp.exp(log_decay * block)

    def to_blocks(values):
        return jnp.moveaxis(values.reshape(sequences, nblocks, block, heads, head_size), 1, 0)

    def advance(carried, pieces):
        query_blk, key_blk, value_blk = pieces
        scores = jnp.einsum('snhd,smhd->shnm', query_blk, key_blk, precision=highest) * inside
        within = jnp.einsum('shnm,smhe->snhe', scores, value_blk, precision=highest)
        across = jnp.einsum('snhd,shde->snhe', query_blk, carried, precision=highest) * query_decay[None, :, :, None]
        weighted = key_blk * key_decay[None, :, :, None]
        carried = carried * block_decay[None, :, None, None] + jnp.einsum('smhd,smhe->shde', weighted, value_blk, precision=highest)
        return (carried, within + across)
    initial = jnp.zeros((sequences, heads, head_size, head_size), jnp.float32)
    _, results = lax.scan(advance, initial, (to_blocks(queries), to_blocks(keys_all), to_blocks(values_all)))
    results = jnp.moveaxis(results, 0, 1).reshape(sequences, length, heads, head_size)
    results = results * lax.rsqrt(lax.optimization_barrier(jnp.mean(results * results, axis=-1, keepdims=True)) + HEAD_EPS)
    return results.reshape(total_rows, heads * head_size)

def reference(tokens, gain_one, w_gate, w_up, w_down, scale_gate, scale_up, scale_down, gain_mix, w_query, w_key, w_value, w_outgate, scale_query, scale_key, scale_value, scale_outgate, ret_gain, decay_rate, w_mix, scale_mix, gain_two):
    ffn_one = feed_forward(rms_rows(tokens, gain_one), w_gate, w_up, w_down, scale_gate, scale_up, scale_down)
    first = (tokens.astype(jnp.float32) + 0.5 * ffn_one).astype(jnp.bfloat16)
    features = rms_rows(first, gain_mix)
    query_rows = project(features, w_query, scale_query).astype(jnp.bfloat16)
    key_rows = project(features, w_key, scale_key).astype(jnp.bfloat16)
    value_rows = project(features, w_value, scale_value).astype(jnp.bfloat16)
    outgate_rows = project(features, w_outgate, scale_outgate).astype(jnp.bfloat16)
    retained = retain(query_rows, key_rows, value_rows, decay_rate, LEN, BLK)
    mixed = (retained * ret_gain * jax.nn.silu(outgate_rows.astype(jnp.float32))).astype(jnp.bfloat16)
    second = (first.astype(jnp.float32) + split_sum(mixed, w_mix, N_TP) * scale_mix).astype(jnp.bfloat16)
    ffn_two = feed_forward(rms_rows(second, gain_two), w_gate, w_up, w_down, scale_gate, scale_up, scale_down)
    return (second.astype(jnp.float32) + 0.5 * ffn_two).astype(jnp.bfloat16)
```

```python
import functools

import jax
import jax.numpy as jnp
import numpy as np
from jax import lax
from jax.experimental import pallas as pl
from jax.experimental.pallas import tpu as pltpu
from jax.sharding import PartitionSpec as P

LEN = 256
EPS = 1e-06
HEAD_EPS = 0.1


def grid_of(count):
    inner = max(d for d in range(1, int(count**0.5) + 1) if count % d == 0)
    return count // inner, inner


def shift(axis, outer, inner, by_outer, by_inner):
    return axis, [
        (o * inner + i, (o + by_outer) % outer * inner + (i + by_inner) % inner)
        for o in range(outer)
        for i in range(inner)
    ]


def send(value, axis, pairs):
    return lax.ppermute(value, axis, pairs)


def ring(pieces, dims, along):
    count = dims[along]
    step = (1, 0) if along == 0 else (0, 1)
    up = shift("fs", *dims, *step)
    down = shift("fs", *dims, -step[0], -step[1])

    def moved(offset, by):
        return tuple((a + by * s) % n for a, s, n in zip(offset, step, dims))

    out = list(pieces)
    for offset, row, array in pieces:
        if count == 1:
            continue
        above = below = array
        half = (count - 1) // 2
        for k in range(1, half + 1):
            above = send(above, *up)
            below = send(below, *down)
            out.append((moved(offset, -k), row, above))
            out.append((moved(offset, k), row, below))
        if count == 2:
            out.append((moved(offset, 1), row, send(array, *up)))
        elif count % 2 == 0:
            mid = array.shape[0] // 2
            out.append((moved(offset, -half - 1), row, send(above[:mid], *up)))
            out.append((moved(offset, half + 1), row + mid, send(below[mid:], *down)))
    return out


def gather_fs(array, dims, order):
    pieces = [((0, 0), 0, array)]
    for along in order:
        pieces = ring(pieces, dims, along)
    return pieces


def gather_tp(piece, tp_dims):
    x_count, cores = tp_dims
    across = [piece] + [
        send(piece, *shift("tp", *tp_dims, -k, 0)) for k in range(1, x_count)
    ]
    out = list(across)
    for k in range(1, cores):
        out += [send(v, *shift("tp", *tp_dims, 0, -k)) for v in across]
    return out


def scatter_tp(outs, tp_dims):
    x_count, cores = tp_dims
    total = outs[0].astype(jnp.float32)
    for k in range(1, cores):
        total = total + send(outs[k], *shift("tp", *tp_dims, 0, k)).astype(jnp.float32)
    mine = total[0]
    low = total.astype(jnp.bfloat16)
    for j in range(1, x_count):
        mine = mine + send(low[j], *shift("tp", *tp_dims, j, 0)).astype(jnp.float32)
    return mine


def silu(v):
    return v / (1.0 + jnp.exp(-v))


def dot(a, b):
    return jnp.dot(a, b, preferred_element_type=jnp.float32)


def start_copies(place, segs_a, segs_b, refs, wa, wb, sems, rows):
    copies = []
    for n, ((slot, row, size), ref) in enumerate(zip(segs_a + segs_b, refs)):
        into = wa if n < len(segs_a) else wb
        first = pl.multiple_of(place[slot] * rows + row, 16)
        copies.append(pltpu.make_async_copy(ref, into.at[pl.ds(first, size)], sems.at[n]))
    for c in copies:
        c.start()
    return copies


def normed(place, base, x_refs, gain, xs, width):
    total = 0.0
    for ref in x_refs:
        v = ref[...].astype(jnp.float32)
        total = total + jnp.sum(v * v, axis=1, keepdims=True)
    scale = lax.rsqrt(total / (width * len(x_refs)) + EPS)
    for r, ref in enumerate(x_refs):
        v = ref[...].astype(jnp.float32) * scale * gain[r : r + 1, :]
        xs[place[base + r]] = v.astype(jnp.bfloat16)


def project(xs, weight, lo, hi):
    tps, _, width = xs.shape
    acc = dot(xs[0], weight[0:width, lo:hi])
    for t in range(1, tps):
        acc = acc + dot(xs[t], weight[t * width : (t + 1) * width, lo:hi])
    return acc


def write_out(place, base, left, downs, out, rows, width):
    cores, x_count = out.shape[:2]
    for c in range(cores):
        for x in range(x_count):
            owner = place[base + c * x_count + x]
            for b in range(width // rows):
                first = pl.multiple_of(owner * width + b * rows, 16)
                acc = 0.0
                for n, (weight, lo) in enumerate(downs):
                    acc = acc + dot(
                        left[:, n * rows : (n + 1) * rows],
                        weight[pl.ds(first, rows), lo : lo + rows],
                    )
                out[c, x, :, b * rows : (b + 1) * rows] = acc.astype(jnp.bfloat16)


def ffn_kernel(place, *refs, base, tps, segs_a, segs_b, rows, cut):
    x_refs = refs[:tps]
    gain, scale_gate, scale_up = refs[tps : tps + 3]
    seg_refs = refs[tps + 3 : tps + 3 + len(segs_a) + len(segs_b)]
    out, xs, wa, wb, sems = refs[-5:]
    copies = start_copies(place, segs_a, segs_b, seg_refs, wa, wb, sems, rows)
    width = xs.shape[2]
    normed(place, base, x_refs, gain, xs, width)
    for c in copies:
        c.wait()
    hid = scale_gate.shape[1]
    gate = project(xs, wa, 0, hid) * scale_gate[...]
    up = project(xs, wb, 0, hid) * scale_up[...]
    hidden = (silu(gate) * up).astype(jnp.bfloat16)
    downs = [
        (wa, hid + n * rows) if n < cut else (wb, hid + (n - cut) * rows)
        for n in range(hid // rows)
    ]
    write_out(place, base, hidden, downs, out, rows, width)


def mix_kernel(place, rate, *refs, base, tps, segs_a, segs_b, rows):
    x_refs = refs[:tps]
    gain, scales, ret_gain, cosines, sines = refs[tps : tps + 5]
    seg_refs = refs[tps + 5 : tps + 5 + len(segs_a) + len(segs_b)]
    out, xs, wa, wb, sems = refs[-5:]
    copies = start_copies(place, segs_a, segs_b, seg_refs, wa, wb, sems, rows)
    width = xs.shape[2]
    normed(place, base, x_refs, gain, xs, width)
    for c in copies:
        c.wait()
    rw = ret_gain.shape[1]
    query = (project(xs, wa, 0, rw) * scales[0:1, :]).astype(jnp.bfloat16)
    key = (project(xs, wa, rw, 2 * rw) * scales[1:2, :]).astype(jnp.bfloat16)
    value = (project(xs, wb, 0, rw) * scales[2:3, :]).astype(jnp.bfloat16)
    outgate = (project(xs, wb, rw, 2 * rw) * scales[3:4, :]).astype(jnp.bfloat16)
    heads = rate.shape[0]
    size = rw // heads
    length = xs.shape[1]
    at = lax.broadcasted_iota(jnp.int32, (size, size), 0)
    to = lax.broadcasted_iota(jnp.int32, (size, size), 1)
    even = to % 2 == 0
    minus = jnp.where(even & (at == to + 1), -1.0, 0.0)
    turn = jnp.where((~even) & (at == to - 1), 1.0, minus).astype(jnp.bfloat16)
    far = lax.broadcasted_iota(jnp.int32, (length, length), 0) - lax.broadcasted_iota(
        jnp.int32, (length, length), 1
    )
    distance = jnp.maximum(far, 0).astype(jnp.float32)

    def turned(v):
        return v.astype(jnp.float32) * cosines[...] + dot(v, turn) * sines[...]

    mixed = []
    for h in range(heads):
        cols = slice(h * size, (h + 1) * size)
        q = turned(query[:, cols]).astype(jnp.bfloat16)
        k = (turned(key[:, cols]) * size**-0.5).astype(jnp.bfloat16)
        scores = lax.dot_general(
            q, k, (((1,), (1,)), ((), ())), preferred_element_type=jnp.float32
        )
        inside = jnp.where(far >= 0, jnp.exp(-rate[h] * distance), 0.0)
        held = dot((scores * inside).astype(jnp.bfloat16), value[:, cols])
        held = held * lax.rsqrt(jnp.mean(held * held, axis=1, keepdims=True) + HEAD_EPS)
        gate = silu(outgate[:, cols].astype(jnp.float32))
        mixed.append((held * ret_gain[:, cols] * gate).astype(jnp.bfloat16))
    mixed = jnp.concatenate(mixed, axis=1) if heads > 1 else mixed[0]
    downs = [(wb, 2 * rw + n * rows) for n in range(rw // rows)]
    write_out(place, base, mixed, downs, out, rows, width)


def call(kernel, name, place, smem, xs, small, pieces_a, pieces_b, dims, tp_dims, **kw):
    x_count, cores = tp_dims
    tps = x_count * cores
    length, width = xs[0].shape
    rows = pieces_a[0][2].shape[0]

    def segs(pieces):
        return [(o[0] * dims[1] + o[1], row, a.shape[0]) for o, row, a in pieces]

    segs_a, segs_b = segs(pieces_a), segs(pieces_b)
    arrays = [p[2] for p in pieces_a + pieces_b]
    full = rows * dims[0] * dims[1]
    vm = pl.BlockSpec(memory_space=pltpu.VMEM)
    sm = pl.BlockSpec(memory_space=pltpu.SMEM)
    anywhere = pl.BlockSpec(memory_space=pl.ANY)
    cols_a, cols_b = pieces_a[0][2].shape[1], pieces_b[0][2].shape[1]
    body = functools.partial(
        kernel,
        base=dims[0] * dims[1],
        tps=tps,
        segs_a=segs_a,
        segs_b=segs_b,
        rows=rows,
        **kw,
    )
    return pl.pallas_call(
        body,
        name=name,
        out_shape=jax.ShapeDtypeStruct((cores, x_count, length, width), jnp.bfloat16),
        in_specs=[sm] * (1 + len(smem))
        + [vm] * (len(xs) + len(small))
        + [anywhere] * len(arrays),
        out_specs=vm,
        scratch_shapes=[
            pltpu.VMEM((tps, length, width), jnp.bfloat16),
            pltpu.VMEM((full, cols_a), jnp.bfloat16),
            pltpu.VMEM((full, cols_b), jnp.bfloat16),
            pltpu.SemaphoreType.DMA((len(arrays),)),
        ],
        cost_estimate=pl.CostEstimate(
            flops=2 * length * full * (cols_a + cols_b),
            bytes_accessed=2 * full * (cols_a + cols_b),
            transcendentals=0,
        ),
        compiler_params=pltpu.CompilerParams(vmem_limit_bytes=40 * 2**20),
    )(place, *smem, *xs, *small, *arrays)


def tables(length, size):
    freq = 1.0 / 10000.0 ** np.linspace(0.0, 1.0, size // 2, dtype=np.float32)
    freq = np.repeat(freq.astype(np.float32), 2)
    angles = np.arange(length, dtype=np.float32)[:, None] * freq[None, :]
    return np.cos(angles).astype(np.float32), np.sin(angles).astype(np.float32)


def per_device(
    tokens,
    gain_one,
    w_gate,
    w_up,
    w_down,
    scale_gate,
    scale_up,
    scale_down,
    gain_mix,
    w_query,
    w_key,
    w_value,
    w_outgate,
    scale_query,
    scale_key,
    scale_value,
    scale_outgate,
    ret_gain,
    decay_rate,
    w_mix,
    scale_mix,
    gain_two,
    *,
    fs,
    tp,
):
    dims = grid_of(fs)
    cores = 2 if tp % 2 == 0 else 1
    tp_dims = (tp // cores, cores)
    low = jnp.bfloat16
    rows = w_gate.shape[0]
    size = w_query.shape[1] // decay_rate.shape[0]

    mine = lax.axis_index("fs").astype(jnp.int32)
    n = jnp.arange(fs, dtype=jnp.int32)
    fs_at = (mine // dims[1] + n // dims[1]) % dims[0] * dims[1] + (
        mine % dims[1] + n % dims[1]
    ) % dims[1]
    own = lax.axis_index("tp").astype(jnp.int32)
    m = jnp.arange(tp, dtype=jnp.int32)
    tp_at = (own // cores + m % tp_dims[0]) % tp_dims[0] * cores + (
        own % cores + m // tp_dims[0]
    ) % cores
    place = jnp.concatenate([fs_at, tp_at])

    hid = w_gate.shape[1]
    downs = [w_down[k * rows : (k + 1) * rows].astype(low) for k in range(hid // rows)]
    cut = len(downs) * 4 // 9
    group_a = jnp.concatenate([w_gate.astype(low)] + downs[:cut], axis=1)
    group_b = jnp.concatenate([w_up.astype(low)] + downs[cut:], axis=1)
    ffn_a = gather_fs(group_a, dims, (0, 1))
    ffn_b = gather_fs(group_b, dims, (1, 0))

    held = lax.optimization_barrier(
        (w_query, w_key, w_value, w_outgate, w_mix, ffn_a[-3][2], ffn_b[-3][2])
    )
    w_query, w_key, w_value, w_outgate, w_mix = held[:5]
    ffn_a[-3] = ffn_a[-3][:2] + (held[5],)
    ffn_b[-3] = ffn_b[-3][:2] + (held[6],)
    mixes = [
        w_mix[k * rows : (k + 1) * rows].astype(low) for k in range(w_mix.shape[0] // rows)
    ]
    mix_a = gather_fs(
        jnp.concatenate([w_query.astype(low), w_key.astype(low)], axis=1), dims, (0, 1)
    )
    mix_b = gather_fs(
        jnp.concatenate([w_value.astype(low), w_outgate.astype(low)] + mixes, axis=1),
        dims,
        (1, 0),
    )

    gains = jnp.stack([gain_one, gain_mix, gain_two])
    gains = jnp.stack(gather_tp(gains, tp_dims), axis=1)
    scales = jnp.stack([scale_query, scale_key, scale_value, scale_outgate])
    cosines, sines = tables(LEN, size)

    def ffn(value, which):
        outs = call(
            ffn_kernel,
            "ffn",
            place,
            [],
            gather_tp(value, tp_dims),
            [gains[which], scale_gate[None], scale_up[None]],
            ffn_a,
            ffn_b,
            dims,
            tp_dims,
            cut=cut,
        )
        total = scatter_tp(outs, tp_dims)
        return (value.astype(jnp.float32) + 0.5 * total * scale_down).astype(low)

    def mixing(value):
        outs = call(
            mix_kernel,
            "mix",
            place,
            [decay_rate],
            gather_tp(value, tp_dims),
            [gains[1], scales, ret_gain[None], cosines, sines],
            mix_a,
            mix_b,
            dims,
            tp_dims,
        )
        total = scatter_tp(outs, tp_dims)
        return (value.astype(jnp.float32) + total * scale_mix).astype(low)

    chunks = [tokens[s : s + LEN] for s in range(0, tokens.shape[0], LEN)]
    chunks = [ffn(c, 0) for c in chunks]
    chunks = [mixing(c) for c in chunks]
    chunks = [ffn(c, 2) for c in chunks]
    return jnp.concatenate(chunks, axis=0)


def solution(mesh):
    both, one = P("fs", "tp"), P("tp")
    flipped = P("tp", "fs")
    return jax.shard_map(
        functools.partial(per_device, fs=mesh.shape["fs"], tp=mesh.shape["tp"]),
        mesh=mesh,
        in_specs=(both, one, both, both, flipped)
        + (one,) * 4
        + (both,) * 4
        + (one,) * 6
        + (flipped, one, one),
        out_specs=both,
        check_vma=False,
    )
```
